32 devices in a mesh: ep: 8 (over z, x), tp: 4 (over y, core).
Axes of the slice: x: 2, y: 2, z: 4, core: 2. Of those that a mesh axis runs over, the one named last changes fastest.
Arguments:
- projected_queries: bfloat16 [2048, 2048], P('ep', 'tp'), may hold values from -245 to 245, as said below
- key_proj: bfloat16 [2048, 512], P('ep', 'tp'), may hold values from -6.2 to 6.2
- projected_values: bfloat16 [2048, 512], P('ep', 'tp'), may hold values from -24 to 24
- head_sink_logits: float32 [32], P('tp'), may hold values from 1 to 6
- out_weight: bfloat16 [2048, 4096], P('tp'), may hold values from -0.125 to 0.125
- expert_input: bfloat16 [1024, 4096], P('ep'), may hold values from -6 to 6
- norm_gain: float32 [4096], replicated, may hold values from 0.1 to 1.9
- routing: int32 [1024, 4], P('ep'), may hold values from 0 to 7, all different within a row; in each aligned block of 128 rows (0 to 127, 128 to 255, ...) at most 96 rows name the same one
- route_weight: float32 [1024, 4], P('ep'), may hold values from 0.1 to 1
- gate_weight: bfloat16 [8, 4096, 1024], P('ep', None, 'tp'), may hold values from -0.27929688 to 0.27929688
- up_weight: bfloat16 [8, 4096, 1024], P('ep', None, 'tp'), may hold values from -0.27929688 to 0.27929688
- down_weight: bfloat16 [8, 1024, 4096], P('ep', 'tp'), may hold values from -0.046875 to 0.046875
Outputs:
- mixer_output: bfloat16 [2048, 4096], P(('ep', 'tp'))
- expert_output: bfloat16 [1024, 4096], P('ep', 'tp')
The draws below stay inside these ranges and needn't reach their ends.
Inputs may be any that keep to these rules, and one draw needn't show every extreme that they name: `projected_queries`: in the hidden draw some queries nearly equal a large multiple of a nearby key. `routing`: each row names 4 different experts; among the rows of one device (aligned blocks of 128 rows) no expert is named more than 96 times, a bound that some block reaches.
All inputs are finite; a program needn't handle non-finite values.
Results may differ from the reference program's by a relative error of at most 0.014.
Values may be sent and summed in bfloat16 or wider, within the bound.
A program may use at most 128 MiB of HBM per device.

```python
import math
import jax
import jax.numpy as jnp
import numpy as np
from jax import lax

D = 4096
QUERY_HEADS = 32
KEY_VALUE_HEADS = 8
HEAD_SIZE = 64
WINDOW_KEYS = 128
FF = 1024
TOPK = 4
TOK_B_DEV = 128
EXPERTS = 8
CAP = 96
ATTENTION_TOKENS = 2048
TOKENS_B = 1024
N_EP = 8
N_TP = 4


def plant_pair(key):
    base = jax.random.fold_in(key, 17)
    leading_key, following_key = jax.random.split(base, 2)
    sampled_keys = jnp.clip(jax.random.normal(following_key, (ATTENTION_TOKENS, KEY_VALUE_HEADS, HEAD_SIZE), jnp.float32), -6.0, 6.0)
    query_vectors = jnp.clip(jax.random.normal(leading_key, (ATTENTION_TOKENS, KEY_VALUE_HEADS, QUERY_HEADS // KEY_VALUE_HEADS, HEAD_SIZE), jnp.float32), -6.0, 6.0)
    return (query_vectors.reshape(ATTENTION_TOKENS, QUERY_HEADS * HEAD_SIZE), sampled_keys.reshape(ATTENTION_TOKENS, KEY_VALUE_HEADS * HEAD_SIZE))


def draw_projected_queries(key, part):
    return plant_pair(key)[0].astype(jnp.bfloat16)


def draw_key_proj(key, part):
    return plant_pair(key)[1].astype(jnp.bfloat16)


def block_scale(own_key, extent, cuts, smallest, largest):
    factor_of, own = 1.0, jax.random.fold_in(own_key, 6)
    for dim, shards_of in cuts:
        draws = jnp.exp(jax.random.uniform(jax.random.fold_in(own, dim), (shards_of,), jnp.float32, smallest / len(cuts), largest / len(cuts)))
        factor_of = factor_of * jnp.repeat(draws, extent[dim] // shards_of).reshape([-1 if axis == dim else 1 for axis in range(len(extent))])
    return factor_of


def assign_block(key, own, number, rows, number_of, top, bound, skew):
    sequence = jax.random.permutation(key, number_of)
    heavy_load, common = shares(number_of, rows * top, bound, skew, True), shares(number_of, rows * top, bound, skew, False)
    places = jnp.arange(number_of)

    def named(tallies, rotation):
        used = int((tallies > 0).sum())
        fixed = max(1, used // 4)
        moved = fixed + (places - fixed + rotation * (used - fixed)) % max(1, number_of - fixed)
        return jnp.zeros((number_of,), jnp.int32).at[sequence[jnp.where(places < fixed, places, moved)]].set(jnp.asarray(tallies, jnp.int32))

    tallies = jnp.where(number % 4 == 0, named(heavy_load, number // 4), named(common, number - number // 4 - 1))
    mixed = jax.random.permutation(jax.random.fold_in(own, 3), number_of)
    giver, taker = mixed[0:number_of // 2 * 2:2], mixed[1:number_of // 2 * 2:2]
    room = jnp.minimum(tallies[giver] - 1, bound - tallies[taker]) // 2
    room = jnp.where((giver == sequence[0]) | (taker == sequence[0]) | (tallies[taker] == 0), 0, jnp.maximum(room, 0))
    moved = jax.random.randint(jax.random.fold_in(own, 4), (number_of // 2,), 0, 1 << 20) % (room + 1)
    tallies = tallies.at[giver].add(-moved).at[taker].add(moved)
    items = jnp.searchsorted(jnp.cumsum(tallies), jnp.arange(rows * top), side="right").astype(jnp.int32)
    table = items.reshape(top, rows).T
    table = table[jax.random.permutation(jax.random.fold_in(own, 1), rows)]
    rotation = jax.random.randint(jax.random.fold_in(own, 2), (rows, 1), 0, top)
    return jnp.take_along_axis(table, (jnp.arange(top)[None, :] + rotation) % top, axis=1)


def shares(number_of, total, limit, slope, full):
    loads = [(1 << 20) // math.isqrt(rank ** slope) + 1 for rank in range(1, number_of + 1)]
    largest = limit if full else min(limit, max(-(-total // number_of), total * loads[0] // sum(loads)))
    least = 1 if total - largest >= number_of - 1 else 0
    holding, surplus = [largest] + [least] * (number_of - 1), total - largest - least * (number_of - 1)
    while surplus > 0:
        free = [i for i in range(1, number_of) if holding[i] < largest] or [i for i in range(1, number_of) if holding[i] < limit]
        pool, remaining = sum([loads[i] for i in free]), surplus
        for i in free:
            more = min(limit - holding[i], max(1, remaining * loads[i] // pool), surplus)
            holding[i] = holding[i] + more
            surplus = surplus - more
    return np.array(holding)


def scatter_about(stream_key, shape, scale, bound, cuts=(), held_as=jnp.bfloat16):
    gain = block_scale(stream_key, shape, cuts, -0.22, 0.18) if cuts else 1.0
    drawn = jax.random.normal(stream_key, shape, jnp.float32) * scale * gain
    return jnp.minimum(jnp.maximum(drawn, -bound), bound).astype(held_as)


def setup_inputs(seed: int = 0) -> dict:
    arg_keys = jax.random.split(jax.random.key(seed), 13)
    projected_queries = draw_projected_queries(jax.random.fold_in(arg_keys[12], 71), 0)
    key_proj = draw_key_proj(jax.random.fold_in(arg_keys[12], 71), 0)
    projected_values = scatter_about(arg_keys[2], (ATTENTION_TOKENS, KEY_VALUE_HEADS * HEAD_SIZE), 4.0, 24.0, ((0, 8), (1, 4)))
    head_sink_logits = jnp.clip(1.0 + 5.0 * jax.random.uniform(arg_keys[3], (QUERY_HEADS,), jnp.float32) ** block_scale(arg_keys[3], (QUERY_HEADS,), ((0, 4),), -0.2, 0.2), 1.0, 6.0)
    out_weight = scatter_about(arg_keys[4], (QUERY_HEADS * HEAD_SIZE, D), (QUERY_HEADS * HEAD_SIZE) ** -0.5, 0.125, ((0, 4),))
    expert_input = scatter_about(arg_keys[5], (TOKENS_B, D), 1.0, 6.0, ((0, 8),))
    norm_gain = jnp.clip(1.0 + 0.18 * jax.random.normal(arg_keys[6], (D,), jnp.float32), 0.1, 1.9)
    routing_keys = jax.random.split(jax.random.fold_in(arg_keys[7], 1), TOKENS_B // TOK_B_DEV)
    routing_turns = jax.random.permutation(jax.random.fold_in(arg_keys[7], 3), TOKENS_B // TOK_B_DEV)
    routing = jax.vmap(lambda own, number: assign_block(jax.random.fold_in(arg_keys[7], 2), own, number, TOK_B_DEV, N_EP, TOPK, CAP, 2))(routing_keys, routing_turns).reshape((TOKENS_B, TOPK))
    route_weight = jnp.clip(jnp.exp(math.log(1.0) - 2.3025851 * jax.random.uniform(arg_keys[8], (TOKENS_B, TOPK), jnp.float32) ** block_scale(arg_keys[8], (TOKENS_B, TOPK), ((0, 8),), -0.2, 0.2)), 0.1, 1.0)
    gate_weight = scatter_about(arg_keys[9], (EXPERTS, D, FF), 0.046875, 0.27929688, ((0, 8), (2, 4)))
    up_weight = scatter_about(arg_keys[10], (EXPERTS, D, FF), 0.046875, 0.27929688, ((0, 8), (2, 4)))
    down_weight = scatter_about(arg_keys[11], (EXPERTS, FF, D), (16 * FF) ** -0.5, 0.046875, ((0, 8), (1, 4)))
    return {"projected_queries": projected_queries, "key_proj": key_proj, "projected_values": projected_values, "head_sink_logits": head_sink_logits, "out_weight": out_weight, "expert_input": expert_input, "norm_gain": norm_gain, "routing": routing, "route_weight": route_weight, "gate_weight": gate_weight, "up_weight": up_weight, "down_weight": down_weight}


EPS = 1e-06
CLAMP = 7.0
SLOPE = 1.702

def attend_single_head(kernel_inputs, permitted_mask):
    query_head, key_head, value_head, sink_head = kernel_inputs
    scores = jnp.einsum('nqgd,nsd->ngqs', query_head, key_head) * HEAD_SIZE ** (-0.5)
    scores = jnp.where(permitted_mask[:, None, :, :], scores, -jnp.inf)
    sink_col = sink_head[None, :, None, None]
    highest = jnp.maximum(lax.optimization_barrier(jnp.max(scores, axis=-1, keepdims=True)), sink_col)
    numerator = jnp.exp(scores - highest)
    denominator = lax.optimization_barrier(jnp.sum(numerator, axis=-1, keepdims=True)) + jnp.exp(sink_col - highest)
    weights = (numerator / denominator).astype(jnp.bfloat16)
    return jnp.einsum('ngqs,nsd->nqgd', weights.astype(jnp.float32), value_head.astype(jnp.float32))

def slot_targets(flat_ids, capacity):
    onehot = (flat_ids[:, None] == jnp.arange(N_EP, dtype=jnp.int32)[None, :]).astype(jnp.int32)
    rank_in = jnp.cumsum(onehot, axis=0) - 1
    slot_pos = lax.optimization_barrier(jnp.sum(rank_in * onehot, axis=1))
    return (flat_ids * capacity + slot_pos).astype(jnp.int32)

def reference(projected_queries, key_proj, projected_values, head_sink_logits, out_weight, expert_input, norm_gain, routing, route_weight, gate_weight, up_weight, down_weight):
    total = projected_queries.shape[0]
    count_of_blocks = total // WINDOW_KEYS
    heads_per_group = QUERY_HEADS // KEY_VALUE_HEADS
    query_vectors = projected_queries.astype(jnp.float32).reshape(count_of_blocks, WINDOW_KEYS, KEY_VALUE_HEADS, heads_per_group, HEAD_SIZE)
    blank_rows = jnp.zeros((WINDOW_KEYS, KEY_VALUE_HEADS * HEAD_SIZE), jnp.bfloat16)
    padded_keys = jnp.concatenate([blank_rows, key_proj], axis=0).astype(jnp.float32)
    padded_values = jnp.concatenate([blank_rows, projected_values], axis=0)
    window_keys = jnp.concatenate([padded_keys[:-WINDOW_KEYS].reshape(count_of_blocks, WINDOW_KEYS, KEY_VALUE_HEADS, HEAD_SIZE), padded_keys[WINDOW_KEYS:].reshape(count_of_blocks, WINDOW_KEYS, KEY_VALUE_HEADS, HEAD_SIZE)], axis=1)
    window_values = jnp.concatenate([padded_values[:-WINDOW_KEYS].reshape(count_of_blocks, WINDOW_KEYS, KEY_VALUE_HEADS, HEAD_SIZE), padded_values[WINDOW_KEYS:].reshape(count_of_blocks, WINDOW_KEYS, KEY_VALUE_HEADS, HEAD_SIZE)], axis=1)
    block_ids = jnp.arange(count_of_blocks)[:, None, None] * WINDOW_KEYS
    query_pos = block_ids + jnp.arange(WINDOW_KEYS)[None, :, None] + WINDOW_KEYS
    key_pos = block_ids + jnp.arange(2 * WINDOW_KEYS)[None, None, :]
    permitted_mask = (key_pos <= query_pos) & (query_pos - key_pos < WINDOW_KEYS) & (key_pos >= WINDOW_KEYS)
    head_outputs = lax.map(lambda kernel_inputs: attend_single_head(kernel_inputs, permitted_mask), (query_vectors.transpose(2, 0, 1, 3, 4), window_keys.transpose(2, 0, 1, 3), window_values.transpose(2, 0, 1, 3), head_sink_logits.reshape(KEY_VALUE_HEADS, heads_per_group)))
    attended = head_outputs.transpose(1, 2, 0, 3, 4).reshape(total, QUERY_HEADS * HEAD_SIZE).astype(jnp.bfloat16)
    head_share = QUERY_HEADS * HEAD_SIZE // N_TP
    summed = jnp.zeros((total, D), jnp.float32)
    for group in range(N_TP):
        partial_value = jnp.dot(attended[:, group * head_share:(group + 1) * head_share], out_weight[group * head_share:(group + 1) * head_share], preferred_element_type=jnp.float32).astype(jnp.bfloat16)
        summed = summed + lax.optimization_barrier(partial_value).astype(jnp.float32)
    mixer_output = summed.astype(jnp.bfloat16)
    capacity = CAP
    widened = expert_input.astype(jnp.float32)
    normed = (widened * lax.rsqrt(lax.optimization_barrier(jnp.mean(widened * widened, axis=-1, keepdims=True)) + EPS) * norm_gain[None, :]).astype(jnp.bfloat16)
    per_source = TOK_B_DEV * TOPK
    flat_ids = routing.reshape(N_EP, per_source).astype(jnp.int32)
    target = jax.vmap(lambda id_row: slot_targets(id_row, capacity))(flat_ids)
    tok_ids = (jnp.arange(per_source) // TOPK).astype(jnp.int32)
    slot_tok = jax.vmap(lambda tgt_row: jnp.full((N_EP * capacity,), TOK_B_DEV, jnp.int32).at[tgt_row].set(tok_ids))(target)
    extended = jnp.concatenate([normed.reshape(N_EP, TOK_B_DEV, D), jnp.zeros((N_EP, 1, D), jnp.bfloat16)], axis=1)

    def run_expert(expert_id):
        picks = lax.dynamic_slice_in_dim(slot_tok, expert_id * capacity, capacity, 1)
        expert_rows = jax.vmap(lambda block_rows, pick_row: jnp.take(block_rows, pick_row, axis=0))(extended, picks)
        expert_rows = expert_rows.reshape(N_EP * capacity, D)
        gate_pre = jnp.dot(expert_rows, gate_weight[expert_id], preferred_element_type=jnp.float32)
        up_pre = jnp.dot(expert_rows, up_weight[expert_id], preferred_element_type=jnp.float32)
        gate_cut = jnp.minimum(gate_pre, CLAMP)
        activated = ((jnp.clip(up_pre, -CLAMP, CLAMP) + 1.0) * gate_cut * jax.nn.sigmoid(SLOPE * gate_cut)).astype(jnp.bfloat16)
        return jnp.dot(activated, down_weight[expert_id], preferred_element_type=jnp.float32).astype(jnp.bfloat16)
    results = lax.map(run_expert, jnp.arange(N_EP, dtype=jnp.int32))
    source = jnp.arange(N_EP, dtype=jnp.int32)[:, None]
    slot_of = target - flat_ids * capacity
    gather_at = ((flat_ids * N_EP + source) * capacity + slot_of).astype(jnp.int32)
    picked = jnp.take(results.reshape(-1, D), gather_at.reshape(-1), axis=0).astype(jnp.float32)
    picked = picked.reshape(N_EP * TOK_B_DEV, TOPK, D)
    expert_output = lax.optimization_barrier(jnp.sum(picked * route_weight[:, :, None], axis=1)).astype(jnp.bfloat16)
    return (mixer_output, expert_output)
```

```python
import jax
import jax.numpy as jnp
from jax import lax
from jax.experimental import pallas as pl
from jax.experimental.pallas import tpu as pltpu
from jax.sharding import PartitionSpec as P

D = 4096
HEAD_SIZE = 64
WINDOW_KEYS = 128
TOPK = 4


EPS = 1e-06
CLAMP = 7.0
SLOPE = 1.702


def passed_along(block, axis, distance):
    devices = range(lax.axis_size(axis))
    route = [(i - distance, i) for i in devices if i - distance in devices]
    return lax.ppermute(block, axis, route)


LINE = 4
MESH = pl.DeviceIdType.MESH


def chosen(z, values):
    result = jnp.int32(values[0])
    for place in range(1, LINE):
        result = jnp.where(z == place, jnp.int32(values[place]), result)
    return result


def nearest_first(place):
    return sorted(range(LINE), key=lambda other: (abs(other - place), other))


def expert_kernel(
    own_ref,
    share_ref,
    gate_ref,
    up_ref,
    down_ref,
    out_ref,
    rows_ref,
    weight_ref,
    sum_ref,
    core_ref,
    pair_ref,
    side_ref,
    up_line_ref,
    down_line_ref,
    last_ref,
    share_send,
    share_recv,
    line_send,
    line_recv,
    side_send,
    side_recv,
    pair_send,
    pair_recv,
    core_send,
    core_recv,
    back_core_send,
    back_core_recv,
    back_pair_send,
    back_pair_recv,
    back_side_send,
    back_side_recv,
    back_line_send,
    back_line_recv,
    last_send,
    last_recv,
):
    e, t = lax.axis_index("ep"), lax.axis_index("tp")
    z, x, y, c = e // 2, e % 2, t // 2, t % 2
    width = own_ref.shape[1]
    tokens = own_ref.shape[0]
    sibling, partner, beside = (e, y * 2 + 1 - c), (e, (1 - y) * 2 + c), (z * 2 + 1 - x, t)
    above, below = (e + 2, t), (e - 2, t)

    def copy(src, dst, send, recv, to):
        return pltpu.make_async_remote_copy(
            src_ref=src, dst_ref=dst, send_sem=send, recv_sem=recv, device_id=to, device_id_type=MESH
        )

    barrier = pltpu.get_barrier_semaphore()
    for step in range(1, 2 * LINE):
        pl.semaphore_signal(
            barrier, inc=1, device_id=((e + step) % (2 * LINE), t), device_id_type=MESH
        )
    for other in (sibling, partner):
        pl.semaphore_signal(barrier, inc=1, device_id=other, device_id_type=MESH)
    pl.semaphore_wait(barrier, 2 * LINE + 1)

    lone = width * 3 // 16
    both = width // 8
    first = pl.multiple_of(y * (width - 2 * lone) + c * lone, 128)
    middle = pl.multiple_of(2 * lone + c * both, 128)
    other_first = pl.multiple_of((1 - y) * (width - 2 * lone) + c * lone, 128)
    parts = (pl.ds(first, lone), pl.ds(middle, both), pl.ds(other_first, lone))

    def view(block, part):
        return rows_ref.at[block, :, parts[part]]

    def source(block, part, mine):
        return own_ref.at[:, parts[part]] if mine else view(block, part)

    def along(way, at, part, mine, to):
        block = at * 2 + x
        return copy(
            source(block, part, mine), view(block, part),
            line_send.at[way, at, part], line_recv.at[at, part], to,
        )

    def across(at, part, mine):
        block = at * 2 + x
        return copy(
            source(block, part, mine), view(block, part),
            side_send.at[at, part], side_recv.at[at, part], beside,
        )

    def across_in(at, part):
        block = at * 2 + 1 - x
        return copy(
            view(block, part), view(block, part), side_send.at[at, part], side_recv.at[at, part], beside
        )

    def to_partner(block):
        return copy(view(block, 0), view(block, 0), pair_send.at[block], pair_recv.at[block], partner)

    def from_partner(block):
        return copy(view(block, 2), view(block, 2), pair_send.at[block], pair_recv.at[block], partner)

    def to_sibling(block, part):
        return copy(
            view(block, part), view(block, part), core_send.at[block, part], core_recv.at[block, part], sibling
        )

    sibling_parts = (
        pl.ds(pl.multiple_of(y * (width - 2 * lone) + (1 - c) * lone, 128), lone),
        pl.ds(pl.multiple_of(2 * lone + (1 - c) * both, 128), both),
        pl.ds(pl.multiple_of((1 - y) * (width - 2 * lone) + (1 - c) * lone, 128), lone),
    )

    def from_sibling(block, part):
        dst = rows_ref.at[block, :, sibling_parts[part]]
        return copy(dst, dst, core_send.at[block, part], core_recv.at[block, part], sibling)

    def share_copy(step):
        to = (e + step) % (2 * LINE)
        return copy(
            share_ref.at[to], weight_ref.at[e], share_send.at[step], share_recv.at[e], (to, t)
        )

    def share_in(step):
        at = (e + step) % (2 * LINE)
        return copy(share_ref.at[at], weight_ref.at[at], share_send.at[step], share_recv.at[at], (at, t))

    for part in (0, 1):
        @pl.when(z < LINE - 1)
        def _():
            along(0, z, part, True, above).start()

        @pl.when(z > 0)
        def _():
            along(1, z, part, True, below).start()

        across(z, part, True).start()
    for step in range(1, 2 * LINE):
        share_copy(step).start()
    rows_ref[e] = own_ref[...]
    weight_ref[e] = share_ref[e]

    near = [chosen(z, [nearest_first(place)[j] for place in range(LINE)]) for j in range(LINE)]
    sequence = []

    def passed_on(block):
        to_partner(block).start()
        to_sibling(block, 0).start()
        to_sibling(block, 1).start()
        sequence.append(block)

    def settle(block):
        from_partner(block).wait_recv()
        to_sibling(block, 2).start()

    for j in range(1, LINE + 1):
        if j < LINE:
            at = near[j]
            for part in (0, 1):
                along(0, at, part, False, above).wait_recv()

                @pl.when((at < z) & (z < LINE - 1))
                def _():
                    along(0, at, part, False, above).start()

                @pl.when((at > z) & (z > 0))
                def _():
                    along(1, at, part, False, below).start()

                across(at, part, False).start()
            passed_on(at * 2 + x)
            if len(sequence) > 2:
                settle(sequence[len(sequence) - 3])
        for part in (0, 1):
            across_in(near[j - 1], part).wait_recv()
        passed_on(near[j - 1] * 2 + 1 - x)
        if len(sequence) > 2:
            settle(sequence[len(sequence) - 3])
    for block in sequence[-2:]:
        settle(block)
    for step in range(1, 2 * LINE):
        share_in(step).wait_recv()
    for block in sequence:
        for part in range(3):
            from_sibling(block, part).wait_recv()

    quarter = width // 4
    early = quarter * 5 // 8
    late = quarter - early
    mine = pl.multiple_of((y * 2 + c) * quarter, 128)
    theirs = pl.multiple_of(((1 - y) * 2 + c) * quarter, 128)
    early_mine, early_theirs = pl.ds(mine, early), pl.ds(theirs, early)
    late_mine = pl.ds(pl.multiple_of(mine + early, 128), late)
    late_theirs = pl.ds(pl.multiple_of(theirs + early, 128), late)
    own_quarter, other_quarter = pl.ds(mine, quarter), pl.ds(theirs, quarter)
    sent_quarters = [
        pl.ds(pl.multiple_of((half * 2 + 1 - c) * quarter, 128), quarter) for half in range(2)
    ]
    kept_quarters = [
        pl.ds(pl.multiple_of((half * 2 + c) * quarter, 128), quarter) for half in range(2)
    ]
    trio = ((early_mine, 0, early), (late_mine, early, late), (late_theirs, quarter, late))

    def add(block, columns, arrived):
        total = sum_ref[block, :, columns].astype(jnp.float32)
        sum_ref[block, :, columns] = (total + arrived.astype(jnp.float32)).astype(jnp.bfloat16)

    def far(j):
        result = chosen(z, [nearest_first(place)[::-1][0] for place in range(LINE)])
        for index in range(1, LINE):
            value = chosen(z, [nearest_first(place)[::-1][index] for place in range(LINE)])
            result = jnp.where(j == index, value, result)
        return result

    def back_core(block, half, columns):
        return copy(
            sum_ref.at[block, :, columns], core_ref.at[block, :, pl.ds(half * quarter, quarter)],
            back_core_send.at[block, half], back_core_recv.at[block, half], sibling,
        )

    def back_pair(block):
        return copy(
            sum_ref.at[block, :, early_theirs], pair_ref.at[block],
            back_pair_send.at[block], back_pair_recv.at[block], partner,
        )

    def back_side(at, index):
        columns, start, length = trio[index]
        return copy(
            sum_ref.at[at * 2 + 1 - x, :, columns], side_ref.at[at, :, pl.ds(start, length)],
            back_side_send.at[at, index], back_side_recv.at[at, index], beside,
        )

    def back_line(way, at, index, to):
        columns, start, length = trio[index]
        landing = (up_line_ref, down_line_ref)[way]
        return copy(
            sum_ref.at[at * 2 + x, :, columns], landing.at[at, :, pl.ds(start, length)],
            back_line_send.at[at, index], back_line_recv.at[way, at, index], to,
        )

    def line_in(way, at):
        for index, (columns, start, length) in enumerate(trio):
            back_line(way, at, index, above).wait_recv()
            landing = (up_line_ref, down_line_ref)[way]
            add(at * 2 + x, columns, landing[at, :, start : start + length])

    last = copy(sum_ref.at[e, :, late_theirs], last_ref, last_send, last_recv, partner)

    def experts_of(block):
        rows = rows_ref[block]
        gate_pre = jnp.dot(rows, gate_ref[...], preferred_element_type=jnp.float32)
        up_pre = jnp.dot(rows, up_ref[...], preferred_element_type=jnp.float32)
        gate_cut = jnp.minimum(gate_pre, CLAMP)
        activated = (
            (jnp.clip(up_pre, -CLAMP, CLAMP) + 1.0) * gate_cut * jax.nn.sigmoid(SLOPE * gate_cut)
        ).astype(jnp.bfloat16)
        weight = jnp.broadcast_to(weight_ref[block][0:1], (tokens, tokens)).T[:, 0:1]

        for place in range(0, width, quarter):
            result = jnp.dot(
                activated, down_ref[:, place : place + quarter], preferred_element_type=jnp.float32
            )
            sum_ref[block, :, place : place + quarter] = (result * weight).astype(jnp.bfloat16)

    def turn(i, carry):
        @pl.when(i < LINE)
        def _():
            at = far(i)

            def one(index, inner):
                block = at * 2 + (1 - x) * (1 - index) + x * index
                experts_of(block)
                for half in range(2):
                    back_core(block, half, sent_quarters[half]).start()
                return inner

            lax.fori_loop(0, 2, one, 0)

        @pl.when((i >= 1) & (i < LINE + 1))
        def _():
            at = far(i - 1)

            def one(index, inner):
                block = at * 2 + (1 - x) * (1 - index) + x * index
                for half in range(2):
                    back_core(block, half, sent_quarters[half]).wait_recv()
                    add(block, kept_quarters[half], core_ref[block, :, half * quarter : (half + 1) * quarter])
                back_pair(block).start()
                return inner

            lax.fori_loop(0, 2, one, 0)

        @pl.when((i >= 2) & (i < LINE + 2))
        def _():
            at = far(i - 2)

            def one(index, inner):
                block = at * 2 + (1 - x) * (1 - index) + x * index
                back_pair(block).wait_recv()
                add(block, early_mine, pair_ref[block])

                @pl.when(index == 0)
                def _():
                    for part in range(3):
                        back_side(at, part).start()

                return inner

            lax.fori_loop(0, 2, one, 0)

        @pl.when(i >= 3)
        def _():
            at = far(i - 3)
            for part, (columns, start, length) in enumerate(trio):
                back_side(at, part).wait_recv()
                add(at * 2 + x, columns, side_ref[at, :, start : start + length])

            @pl.when((at >= z) & (z > 0))
            def _():
                line_in(0, at)

            @pl.when((at <= z) & (z < LINE - 1))
            def _():
                line_in(1, at)

            @pl.when(at > z)
            def _():
                for part in range(3):
                    back_line(0, at, part, above).start()

            @pl.when(at < z)
            def _():
                for part in range(3):
                    back_line(1, at, part, below).start()

        return carry

    lax.fori_loop(0, LINE + 3, turn, 0)
    last.start()
    last.wait_recv()
    out_ref[:, 0:early] = sum_ref[e, :, early_mine]
    closing = sum_ref[e, :, late_mine].astype(jnp.float32) + last_ref[...].astype(jnp.float32)
    out_ref[:, early:quarter] = closing.astype(jnp.bfloat16)

    last.wait_send()
    for part in (0, 1):
        @pl.when(z < LINE - 1)
        def _():
            along(0, z, part, True, above).wait_send()

        @pl.when(z > 0)
        def _():
            along(1, z, part, True, below).wait_send()

        across(z, part, True).wait_send()
    for step in range(1, 2 * LINE):
        share_copy(step).wait_send()
    for j in range(1, LINE):
        at = near[j]
        for part in (0, 1):
            @pl.when((at < z) & (z < LINE - 1))
            def _():
                along(0, at, part, False, above).wait_send()

            @pl.when((at > z) & (z > 0))
            def _():
                along(1, at, part, False, below).wait_send()

            across(at, part, False).wait_send()
    for block in sequence:
        to_partner(block).wait_send()
        for part in range(3):
            to_sibling(block, part).wait_send()

    def drained(at, carry):
        for side in range(2):
            for half in range(2):
                back_core(at * 2 + side, half, sent_quarters[half]).wait_send()
            back_pair(at * 2 + side).wait_send()
        for part in range(3):
            back_side(at, part).wait_send()

            @pl.when(at != z)
            def _():
                back_line(0, at, part, above).wait_send()

        return carry

    lax.fori_loop(0, LINE, drained, 0)


def expert_call(normed, share_of, gate_one, up_one, down_one):
    tokens, width = normed.shape
    quarter = width // 4
    early = quarter * 5 // 8
    carried = quarter + quarter - early
    blocks = 2 * LINE
    kept = jnp.bfloat16
    dma = pltpu.SemaphoreType.DMA
    return pl.pallas_call(
        expert_kernel,
        out_shape=jax.ShapeDtypeStruct((tokens, quarter), jnp.bfloat16),
        in_specs=[pl.BlockSpec(memory_space=pltpu.VMEM)] * 5,
        out_specs=pl.BlockSpec(memory_space=pltpu.VMEM),
        scratch_shapes=[
            pltpu.VMEM((blocks, tokens, width), kept),
            pltpu.VMEM((blocks, 8, tokens), jnp.float32),
            pltpu.VMEM((blocks, tokens, width), kept),
            pltpu.VMEM((blocks, tokens, 2 * quarter), kept),
            pltpu.VMEM((blocks, tokens, early), kept),
            pltpu.VMEM((LINE, tokens, carried), kept),
            pltpu.VMEM((LINE, tokens, carried), kept),
            pltpu.VMEM((LINE, tokens, carried), kept),
            pltpu.VMEM((tokens, quarter - early), kept),
            dma((blocks,)),
            dma((blocks,)),
            dma((2, LINE, 2)),
            dma((LINE, 2)),
            dma((LINE, 2)),
            dma((LINE, 2)),
            dma((blocks,)),
            dma((blocks,)),
            dma((blocks, 3)),
            dma((blocks, 3)),
            dma((blocks, 2)),
            dma((blocks, 2)),
            dma((blocks,)),
            dma((blocks,)),
            dma((LINE, 3)),
            dma((LINE, 3)),
            dma((LINE, 3)),
            dma((2, LINE, 3)),
            dma,
            dma,
        ],
        compiler_params=pltpu.CompilerParams(
            collective_id=0, has_side_effects=True, vmem_limit_bytes=60 * 1024 * 1024
        ),
        cost_estimate=pl.CostEstimate(
            flops=6 * blocks * tokens * width * gate_one.shape[1],
            bytes_accessed=8 * width * gate_one.shape[1],
            transcendentals=0,
        ),
    )(normed, share_of, gate_one, up_one, down_one)


def shards(
    projected_queries,
    key_proj,
    projected_values,
    head_sink_logits,
    out_weight,
    expert_input,
    norm_gain,
    routing,
    route_weight,
    gate_weight,
    up_weight,
    down_weight,
):
    query_rows = projected_queries.shape[0]
    kv_heads = key_proj.shape[1] // HEAD_SIZE
    heads_per_group = projected_queries.shape[1] // HEAD_SIZE // kv_heads
    count_of_blocks = query_rows // WINDOW_KEYS
    prior_key, prior_value = passed_along(
        (key_proj[query_rows - WINDOW_KEYS :], projected_values[query_rows - WINDOW_KEYS :]),
        "ep",
        1,
    )
    key_all = jnp.concatenate([prior_key, key_proj], axis=0)
    value_all = jnp.concatenate([prior_value, projected_values], axis=0)
    window_keys = jnp.concatenate(
        [
            key_all[:-WINDOW_KEYS].reshape(count_of_blocks, WINDOW_KEYS, kv_heads, HEAD_SIZE),
            key_all[WINDOW_KEYS:].reshape(count_of_blocks, WINDOW_KEYS, kv_heads, HEAD_SIZE),
        ],
        axis=1,
    )
    window_values = jnp.concatenate(
        [
            value_all[:-WINDOW_KEYS].reshape(count_of_blocks, WINDOW_KEYS, kv_heads, HEAD_SIZE),
            value_all[WINDOW_KEYS:].reshape(count_of_blocks, WINDOW_KEYS, kv_heads, HEAD_SIZE),
        ],
        axis=1,
    )
    query_blocks = projected_queries.reshape(
        count_of_blocks, WINDOW_KEYS, kv_heads, heads_per_group, HEAD_SIZE
    )
    scores = jnp.einsum(
        "nqhgd,nshd->nhgqs", query_blocks, window_keys, preferred_element_type=jnp.float32
    ) * HEAD_SIZE ** (-0.5)
    offset = lax.axis_index("ep") * query_rows
    block_ids = jnp.arange(count_of_blocks)[:, None, None] * WINDOW_KEYS + offset
    query_pos = block_ids + jnp.arange(WINDOW_KEYS)[None, :, None]
    key_pos = block_ids - WINDOW_KEYS + jnp.arange(2 * WINDOW_KEYS)[None, None, :]
    permitted_mask = (key_pos <= query_pos) & (query_pos - key_pos < WINDOW_KEYS) & (key_pos >= 0)
    scores = jnp.where(permitted_mask[:, None, None, :, :], scores, -jnp.inf)
    sink_col = head_sink_logits.reshape(kv_heads, heads_per_group)[None, :, :, None, None]
    highest = jnp.maximum(jnp.max(scores, axis=-1, keepdims=True), sink_col)
    numerator = jnp.exp(scores - highest)
    denominator = jnp.sum(numerator, axis=-1, keepdims=True) + jnp.exp(sink_col - highest)
    weights = (numerator / denominator).astype(jnp.bfloat16)
    attended = jnp.einsum(
        "nhgqs,nshd->nqhgd", weights, window_values, preferred_element_type=jnp.float32
    )
    attended = attended.astype(jnp.bfloat16).reshape(
        query_rows, kv_heads * heads_per_group * HEAD_SIZE
    )
    mixer_output = lax.psum_scatter(
        jnp.dot(attended, out_weight, preferred_element_type=jnp.float32).astype(jnp.bfloat16),
        "tp",
        scatter_dimension=0,
        tiled=True,
    )
    token_rows = expert_input.shape[0]
    experts = lax.axis_size("ep")
    capacity = max(3 * token_rows * TOPK // (2 * experts), 2)
    col_share = D // lax.axis_size("tp")
    widened = expert_input.astype(jnp.float32)
    normed = (
        widened
        * lax.rsqrt(jnp.mean(widened * widened, axis=-1, keepdims=True) + EPS)
        * norm_gain[None, :]
    ).astype(jnp.bfloat16)
    if (experts, lax.axis_size("tp")) != (2 * LINE, 4) or token_rows % 16:
        flat_ids = routing.reshape(-1)
        onehot = (flat_ids[:, None] == jnp.arange(experts, dtype=jnp.int32)[None, :]).astype(jnp.int32)
        rank_in = jnp.cumsum(onehot, axis=0) - 1
        target = flat_ids * capacity + jnp.sum(rank_in * onehot, axis=1)
        tok_ids = jnp.arange(token_rows * TOPK) // TOPK
        slot_tok = jnp.full((experts * capacity,), token_rows, jnp.int32).at[target].set(tok_ids)
        gate_one = gate_weight[0]
        up_one = up_weight[0]
        own_cols = lax.dynamic_slice_in_dim(normed, lax.axis_index("tp") * col_share, col_share, 1)
        extended = jnp.concatenate([own_cols, jnp.zeros((1, col_share), jnp.bfloat16)], axis=0)
        outgoing = jnp.take(extended, slot_tok, axis=0).reshape(experts, capacity, col_share)
        arrived = lax.all_to_all(outgoing, "ep", split_axis=0, concat_axis=0, tiled=True).reshape(
            experts * capacity, col_share
        )
        portion = lax.all_gather(arrived, "tp", axis=1, tiled=True)
        gate_pre = jnp.dot(portion, gate_one, preferred_element_type=jnp.float32)
        up_pre = jnp.dot(portion, up_one, preferred_element_type=jnp.float32)
        gate_cut = jnp.minimum(gate_pre, CLAMP)
        activated = (
            (jnp.clip(up_pre, -CLAMP, CLAMP) + 1.0) * gate_cut * jax.nn.sigmoid(SLOPE * gate_cut)
        ).astype(jnp.bfloat16)
        partial_value = jnp.dot(activated, down_weight[0], preferred_element_type=jnp.float32)
        expert_result = lax.psum_scatter(
            partial_value.astype(jnp.bfloat16), "tp", scatter_dimension=1, tiled=True
        )
        returned = lax.all_to_all(
            expert_result.reshape(experts, capacity, col_share),
            "ep",
            split_axis=0,
            concat_axis=0,
            tiled=True,
        )
        picked = jnp.take(returned.reshape(experts * capacity, col_share), target, axis=0)
        picked = picked.astype(jnp.float32).reshape(token_rows, TOPK, col_share)
        expert_output = jnp.sum(picked * route_weight[:, :, None], axis=1).astype(jnp.bfloat16)
    else:
        named = routing == lax.broadcasted_iota(jnp.int32, (experts, 1, 1), 0)
        share_of = jnp.sum(jnp.where(named, route_weight[None], 0.0), axis=2)
        share_of = jnp.broadcast_to(share_of[:, None, :], (experts, 8, token_rows))
        expert_output = expert_call(
            normed, share_of, gate_weight[0], up_weight[0], down_weight[0]
        )
    return (mixer_output, expert_output)


def solution(mesh):
    placed = (
        P("ep", "tp"),
        P("ep", "tp"),
        P("ep", "tp"),
        P("tp"),
        P("tp", None),
        P("ep", None),
        P(),
        P("ep", None),
        P("ep", None),
        P("ep", None, "tp"),
        P("ep", None, "tp"),
        P("ep", "tp", None),
    )
    return jax.shard_map(
        shards,
        mesh=mesh,
        in_specs=placed,
        out_specs=(P(("ep", "tp"), None), P("ep", "tp")),
        check_vma=False,
    )
```

```python
import jax
import jax.numpy as jnp
from jax import lax
from jax.experimental import pallas as pl
from jax.experimental.pallas import tpu as pltpu
from jax.sharding import PartitionSpec as P

D = 4096
HEAD_SIZE = 64
WINDOW_KEYS = 128
TOPK = 4


EPS = 1e-06
CLAMP = 7.0
SLOPE = 1.702


def passed_along(block, axis, distance):
    devices = range(lax.axis_size(axis))
    route = [(i - distance, i) for i in devices if i - distance in devices]
    return lax.ppermute(block, axis, route)


LINE = 4
MESH = pl.DeviceIdType.MESH


def chosen(z, values):
    result = jnp.int32(values[0])
    for place in range(1, LINE):
        result = jnp.where(z == place, jnp.int32(values[place]), result)
    return result


def nearest_first(place):
    return sorted(range(LINE), key=lambda other: (abs(other - place), other))


def layer_kernel(
    own_ref,
    share_ref,
    gate_hbm,
    up_hbm,
    down_hbm,
    query_ref,
    key_ref,
    value_ref,
    sink_ref,
    project_hbm,
    mixer_ref,
    out_ref,
    gate_ref,
    up_ref,
    down_ref,
    project_ref,
    halo_ref,
    attended_ref,
    mixed_ref,
    mixed_core_ref,
    mixed_pair_ref,
    load_sem,
    halo_send,
    halo_recv,
    mixed_core_send,
    mixed_core_recv,
    mixed_pair_send,
    mixed_pair_recv,
    rows_ref,
    weight_ref,
    sum_ref,
    core_ref,
    pair_ref,
    side_ref,
    up_line_ref,
    down_line_ref,
    last_ref,
    share_send,
    share_recv,
    line_send,
    line_recv,
    side_send,
    side_recv,
    pair_send,
    pair_recv,
    core_send,
    core_recv,
    back_core_send,
    back_core_recv,
    back_pair_send,
    back_pair_recv,
    back_side_send,
    back_side_recv,
    back_line_send,
    back_line_recv,
    last_send,
    last_recv,
):
    e, t = lax.axis_index("ep"), lax.axis_index("tp")
    z, x, y, c = e // 2, e % 2, t // 2, t % 2
    width = own_ref.shape[1]
    tokens = own_ref.shape[0]
    sibling, partner, beside = (e, y * 2 + 1 - c), (e, (1 - y) * 2 + c), (z * 2 + 1 - x, t)
    above, below = (e + 2, t), (e - 2, t)

    def copy(src, dst, send, recv, to):
        return pltpu.make_async_remote_copy(
            src_ref=src, dst_ref=dst, send_sem=send, recv_sem=recv, device_id=to, device_id_type=MESH
        )

    loads = [
        pltpu.make_async_copy(src, dst, load_sem.at[place])
        for place, (src, dst) in enumerate(
            [(project_hbm, project_ref), (gate_hbm, gate_ref), (up_hbm, up_ref), (down_hbm, down_ref)]
        )
    ]
    for load in loads:
        load.start()
    barrier = pltpu.get_barrier_semaphore()
    for step in range(1, 2 * LINE):
        pl.semaphore_signal(
            barrier, inc=1, device_id=((e + step) % (2 * LINE), t), device_id_type=MESH
        )
    for other in (sibling, partner):
        pl.semaphore_signal(barrier, inc=1, device_id=other, device_id_type=MESH)
    pl.semaphore_wait(barrier, 2 * LINE + 1)

    lone = width * 3 // 16
    both = width // 8
    first = pl.multiple_of(y * (width - 2 * lone) + c * lone, 128)
    middle = pl.multiple_of(2 * lone + c * both, 128)
    other_first = pl.multiple_of((1 - y) * (width - 2 * lone) + c * lone, 128)
    parts = (pl.ds(first, lone), pl.ds(middle, both), pl.ds(other_first, lone))

    def view(block, part):
        return rows_ref.at[block, :, parts[part]]

    def source(block, part, mine):
        return own_ref.at[:, parts[part]] if mine else view(block, part)

    def along(way, at, part, mine, to):
        block = at * 2 + x
        return copy(
            source(block, part, mine), view(block, part),
            line_send.at[way, at, part], line_recv.at[at, part], to,
        )

    def across(at, part, mine):
        block = at * 2 + x
        return copy(
            source(block, part, mine), view(block, part),
            side_send.at[at, part], side_recv.at[at, part], beside,
        )

    def across_in(at, part):
        block = at * 2 + 1 - x
        return copy(
            view(block, part), view(block, part), side_send.at[at, part], side_recv.at[at, part], beside
        )

    def to_partner(block):
        return copy(view(block, 0), view(block, 0), pair_send.at[block], pair_recv.at[block], partner)

    def from_partner(block):
        return copy(view(block, 2), view(block, 2), pair_send.at[block], pair_recv.at[block], partner)

    def to_sibling(block, part):
        return copy(
            view(block, part), view(block, part), core_send.at[block, part], core_recv.at[block, part], sibling
        )

    sibling_parts = (
        pl.ds(pl.multiple_of(y * (width - 2 * lone) + (1 - c) * lone, 128), lone),
        pl.ds(pl.multiple_of(2 * lone + (1 - c) * both, 128), both),
        pl.ds(pl.multiple_of((1 - y) * (width - 2 * lone) + (1 - c) * lone, 128), lone),
    )

    def from_sibling(block, part):
        dst = rows_ref.at[block, :, sibling_parts[part]]
        return copy(dst, dst, core_send.at[block, part], core_recv.at[block, part], sibling)

    def share_copy(step):
        to = (e + step) % (2 * LINE)
        return copy(
            share_ref.at[to], weight_ref.at[e], share_send.at[step], share_recv.at[e], (to, t)
        )

    def share_in(step):
        at = (e + step) % (2 * LINE)
        return copy(share_ref.at[at], weight_ref.at[at], share_send.at[step], share_recv.at[at], (at, t))

    for part in (0, 1):
        @pl.when(z < LINE - 1)
        def _():
            along(0, z, part, True, above).start()

        @pl.when(z > 0)
        def _():
            along(1, z, part, True, below).start()

        across(z, part, True).start()
    queries = query_ref.shape[0]

    def halo_copy(which):
        src = (key_ref, value_ref)[which].at[pl.ds(queries - WINDOW_KEYS, WINDOW_KEYS)]
        to = ((e + 1) % (2 * LINE), t)
        return copy(src, halo_ref.at[which], halo_send.at[which], halo_recv.at[which], to)

    @pl.when(e < 2 * LINE - 1)
    def _():
        halo_copy(0).start()
        halo_copy(1).start()

    @pl.when(e == 0)
    def _():
        halo_ref[...] = jnp.zeros_like(halo_ref)

    for step in range(1, 2 * LINE):
        share_copy(step).start()
    rows_ref[e] = own_ref[...]
    weight_ref[e] = share_ref[e]

    kv_heads = key_ref.shape[1] // HEAD_SIZE
    group = query_ref.shape[1] // HEAD_SIZE // kv_heads
    span = queries // 4
    here = lax.broadcasted_iota(jnp.int32, (WINDOW_KEYS, 2 * WINDOW_KEYS), 0)
    there = lax.broadcasted_iota(jnp.int32, (WINDOW_KEYS, 2 * WINDOW_KEYS), 1)

    def attend(number):
        begin = number * WINDOW_KEYS
        permitted = (there > here) & (there <= here + WINDOW_KEYS)
        if number == 0:
            permitted = permitted & ((there >= WINDOW_KEYS) | (e > 0))
        for kv in range(kv_heads):
            lanes = slice(kv * HEAD_SIZE, (kv + 1) * HEAD_SIZE)
            if number == 0:
                keys = jnp.concatenate([halo_ref[0][:, lanes], key_ref[0:WINDOW_KEYS, lanes]], axis=0)
                values = jnp.concatenate(
                    [halo_ref[1][:, lanes], value_ref[0:WINDOW_KEYS, lanes]], axis=0
                )
            else:
                keys = key_ref[begin - WINDOW_KEYS : begin + WINDOW_KEYS, lanes]
                values = value_ref[begin - WINDOW_KEYS : begin + WINDOW_KEYS, lanes]
            for member in range(group):
                head = kv * group + member
                columns = slice(head * HEAD_SIZE, (head + 1) * HEAD_SIZE)
                scores = lax.dot_general(
                    query_ref[begin : begin + WINDOW_KEYS, columns],
                    keys,
                    (((1,), (1,)), ((), ())),
                    preferred_element_type=jnp.float32,
                ) * HEAD_SIZE ** (-0.5)
                scores = jnp.where(permitted, scores, -jnp.inf)
                sink = sink_ref[head]
                highest = jnp.maximum(jnp.max(scores, axis=-1, keepdims=True), sink)
                numerator = jnp.exp(scores - highest)
                denominator = jnp.sum(numerator, axis=-1, keepdims=True) + jnp.exp(sink - highest)
                weights = (numerator / denominator).astype(jnp.bfloat16)
                found = jnp.dot(weights, values, preferred_element_type=jnp.float32)
                attended_ref[begin : begin + WINDOW_KEYS, columns] = found.astype(jnp.bfloat16)

    def mixed_core(half):
        at = pl.multiple_of((half * 2 + 1 - c) * span, 16)
        return copy(
            mixed_ref.at[pl.ds(at, span)], mixed_core_ref.at[half],
            mixed_core_send.at[half], mixed_core_recv.at[half], sibling,
        )

    mixed_pair = copy(
        mixed_ref.at[pl.ds(pl.multiple_of(((1 - y) * 2 + c) * span, 16), span)], mixed_pair_ref,
        mixed_pair_send, mixed_pair_recv, partner,
    )

    def mixed_rows(half):
        return pl.ds(pl.multiple_of((half * 2 + c) * span, 16), span)

    def mix():
        for number in range(1, queries // WINDOW_KEYS):
            attend(number)

        @pl.when(e > 0)
        def _():
            halo_copy(0).wait_recv()
            halo_copy(1).wait_recv()

        attend(0)
        loads[0].wait()
        for place in range(0, width, width // 4):
            columns = slice(place, place + width // 4)
            mixed_ref[:, columns] = jnp.dot(
                attended_ref[...], project_ref[:, columns], preferred_element_type=jnp.float32
            ).astype(jnp.bfloat16)
        for half in range(2):
            mixed_core(half).start()

    def mix_onward():
        for half in range(2):
            mixed_core(half).wait_recv()
            total = mixed_ref[mixed_rows(half), :].astype(jnp.float32)
            mixed_ref[mixed_rows(half), :] = (
                total + mixed_core_ref[half].astype(jnp.float32)
            ).astype(jnp.bfloat16)
        mixed_pair.start()

    mix()
    near = [chosen(z, [nearest_first(place)[j] for place in range(LINE)]) for j in range(LINE)]
    sequence = []

    def passed_on(block):
        to_partner(block).start()
        to_sibling(block, 0).start()
        to_sibling(block, 1).start()
        sequence.append(block)

    def settle(block):
        from_partner(block).wait_recv()
        to_sibling(block, 2).start()

    for j in range(1, LINE + 1):
        if j < LINE:
            at = near[j]
            for part in (0, 1):
                along(0, at, part, False, above).wait_recv()

                @pl.when((at < z) & (z < LINE - 1))
                def _():
                    along(0, at, part, False, above).start()

                @pl.when((at > z) & (z > 0))
                def _():
                    along(1, at, part, False, below).start()

                across(at, part, False).start()
            passed_on(at * 2 + x)
            if len(sequence) > 2:
                settle(sequence[len(sequence) - 3])
        for part in (0, 1):
            across_in(near[j - 1], part).wait_recv()
        passed_on(near[j - 1] * 2 + 1 - x)
        if len(sequence) > 2:
            settle(sequence[len(sequence) - 3])
    mix_onward()
    for block in sequence[-2:]:
        settle(block)
    for load in loads[1:]:
        load.wait()
    for step in range(1, 2 * LINE):
        share_in(step).wait_recv()
    for block in sequence:
        for part in range(3):
            from_sibling(block, part).wait_recv()

    quarter = width // 4
    early = quarter * 5 // 8
    late = quarter - early
    mine = pl.multiple_of((y * 2 + c) * quarter, 128)
    theirs = pl.multiple_of(((1 - y) * 2 + c) * quarter, 128)
    early_mine, early_theirs = pl.ds(mine, early), pl.ds(theirs, early)
    late_mine = pl.ds(pl.multiple_of(mine + early, 128), late)
    late_theirs = pl.ds(pl.multiple_of(theirs + early, 128), late)
    own_quarter, other_quarter = pl.ds(mine, quarter), pl.ds(theirs, quarter)
    sent_quarters = [
        pl.ds(pl.multiple_of((half * 2 + 1 - c) * quarter, 128), quarter) for half in range(2)
    ]
    kept_quarters = [
        pl.ds(pl.multiple_of((half * 2 + c) * quarter, 128), quarter) for half in range(2)
    ]
    trio = ((early_mine, 0, early), (late_mine, early, late), (late_theirs, quarter, late))

    def add(block, columns, arrived):
        total = sum_ref[block, :, columns].astype(jnp.float32)
        sum_ref[block, :, columns] = (total + arrived.astype(jnp.float32)).astype(jnp.bfloat16)

    def far(j):
        result = chosen(z, [nearest_first(place)[::-1][0] for place in range(LINE)])
        for index in range(1, LINE):
            value = chosen(z, [nearest_first(place)[::-1][index] for place in range(LINE)])
            result = jnp.where(j == index, value, result)
        return result

    def back_core(block, half, columns):
        return copy(
            sum_ref.at[block, :, columns], core_ref.at[block, :, pl.ds(half * quarter, quarter)],
            back_core_send.at[block, half], back_core_recv.at[block, half], sibling,
        )

    def back_pair(block):
        return copy(
            sum_ref.at[block, :, early_theirs], pair_ref.at[block],
            back_pair_send.at[block], back_pair_recv.at[block], partner,
        )

    def back_side(at, index):
        columns, start, length = trio[index]
        return copy(
            sum_ref.at[at * 2 + 1 - x, :, columns], side_ref.at[at, :, pl.ds(start, length)],
            back_side_send.at[at, index], back_side_recv.at[at, index], beside,
        )

    def back_line(way, at, index, to):
        columns, start, length = trio[index]
        landing = (up_line_ref, down_line_ref)[way]
        return copy(
            sum_ref.at[at * 2 + x, :, columns], landing.at[at, :, pl.ds(start, length)],
            back_line_send.at[at, index], back_line_recv.at[way, at, index], to,
        )

    def line_in(way, at):
        for index, (columns, start, length) in enumerate(trio):
            back_line(way, at, index, above).wait_recv()
            landing = (up_line_ref, down_line_ref)[way]
            add(at * 2 + x, columns, landing[at, :, start : start + length])

    last = copy(sum_ref.at[e, :, late_theirs], last_ref, last_send, last_recv, partner)

    def experts_of(block):
        rows = rows_ref[block]
        gate_pre = jnp.dot(rows, gate_ref[...], preferred_element_type=jnp.float32)
        up_pre = jnp.dot(rows, up_ref[...], preferred_element_type=jnp.float32)
        gate_cut = jnp.minimum(gate_pre, CLAMP)
        activated = (
            (jnp.clip(up_pre, -CLAMP, CLAMP) + 1.0) * gate_cut * jax.nn.sigmoid(SLOPE * gate_cut)
        ).astype(jnp.bfloat16)
        weight = jnp.broadcast_to(weight_ref[block][0:1], (tokens, tokens)).T[:, 0:1]

        for place in range(0, width, quarter):
            result = jnp.dot(
                activated, down_ref[:, place : place + quarter], preferred_element_type=jnp.float32
            )
            sum_ref[block, :, place : place + quarter] = (result * weight).astype(jnp.bfloat16)

    def turn(i, carry):
        @pl.when(i < LINE)
        def _():
            at = far(i)

            def one(index, inner):
                block = at * 2 + (1 - x) * (1 - index) + x * index
                experts_of(block)
                for half in range(2):
                    back_core(block, half, sent_quarters[half]).start()
                return inner

            lax.fori_loop(0, 2, one, 0)

        @pl.when((i >= 1) & (i < LINE + 1))
        def _():
            at = far(i - 1)

            def one(index, inner):
                block = at * 2 + (1 - x) * (1 - index) + x * index
                for half in range(2):
                    back_core(block, half, sent_quarters[half]).wait_recv()
                    add(block, kept_quarters[half], core_ref[block, :, half * quarter : (half + 1) * quarter])
                back_pair(block).start()
                return inner

            lax.fori_loop(0, 2, one, 0)

        @pl.when((i >= 2) & (i < LINE + 2))
        def _():
            at = far(i - 2)

            def one(index, inner):
                block = at * 2 + (1 - x) * (1 - index) + x * index
                back_pair(block).wait_recv()
                add(block, early_mine, pair_ref[block])

                @pl.when(index == 0)
                def _():
                    for part in range(3):
                        back_side(at, part).start()

                return inner

            lax.fori_loop(0, 2, one, 0)

        @pl.when(i >= 3)
        def _():
            at = far(i - 3)
            for part, (columns, start, length) in enumerate(trio):
                back_side(at, part).wait_recv()
                add(at * 2 + x, columns, side_ref[at, :, start : start + length])

            @pl.when((at >= z) & (z > 0))
            def _():
                line_in(0, at)

            @pl.when((at <= z) & (z < LINE - 1))
            def _():
                line_in(1, at)

            @pl.when(at > z)
            def _():
                for part in range(3):
                    back_line(0, at, part, above).start()

            @pl.when(at < z)
            def _():
                for part in range(3):
                    back_line(1, at, part, below).start()

        return carry

    lax.fori_loop(0, LINE + 3, turn, 0)
    last.start()
    last.wait_recv()
    out_ref[:, 0:early] = sum_ref[e, :, early_mine]
    closing = sum_ref[e, :, late_mine].astype(jnp.float32) + last_ref[...].astype(jnp.float32)
    out_ref[:, early:quarter] = closing.astype(jnp.bfloat16)

    mixed_pair.wait_recv()
    total = mixed_ref[mixed_rows(y), :].astype(jnp.float32)
    mixer_ref[...] = (total + mixed_pair_ref[...].astype(jnp.float32)).astype(jnp.bfloat16)

    last.wait_send()
    mixed_pair.wait_send()
    for half in range(2):
        mixed_core(half).wait_send()

    @pl.when(e < 2 * LINE - 1)
    def _():
        halo_copy(0).wait_send()
        halo_copy(1).wait_send()

    for part in (0, 1):
        @pl.when(z < LINE - 1)
        def _():
            along(0, z, part, True, above).wait_send()

        @pl.when(z > 0)
        def _():
            along(1, z, part, True, below).wait_send()

        across(z, part, True).wait_send()
    for step in range(1, 2 * LINE):
        share_copy(step).wait_send()
    for j in range(1, LINE):
        at = near[j]
        for part in (0, 1):
            @pl.when((at < z) & (z < LINE - 1))
            def _():
                along(0, at, part, False, above).wait_send()

            @pl.when((at > z) & (z > 0))
            def _():
                along(1, at, part, False, below).wait_send()

            across(at, part, False).wait_send()
    for block in sequence:
        to_partner(block).wait_send()
        for part in range(3):
            to_sibling(block, part).wait_send()

    def drained(at, carry):
        for side in range(2):
            for half in range(2):
                back_core(at * 2 + side, half, sent_quarters[half]).wait_send()
            back_pair(at * 2 + side).wait_send()
        for part in range(3):
            back_side(at, part).wait_send()

            @pl.when(at != z)
            def _():
                back_line(0, at, part, above).wait_send()

        return carry

    lax.fori_loop(0, LINE, drained, 0)


def layer_call(
    normed, share_of, gate_one, up_one, down_one, queries, keys, values, sinks, project
):
    tokens, width = normed.shape
    quarter = width // 4
    early = quarter * 5 // 8
    carried = quarter + quarter - early
    blocks = 2 * LINE
    kept = jnp.bfloat16
    dma = pltpu.SemaphoreType.DMA
    span = queries.shape[0] // 4
    in_vmem = pl.BlockSpec(memory_space=pltpu.VMEM)
    in_smem = pl.BlockSpec(memory_space=pltpu.SMEM)
    stays = pl.BlockSpec(memory_space=pl.ANY)
    return pl.pallas_call(
        layer_kernel,
        out_shape=(
            jax.ShapeDtypeStruct((span, width), kept),
            jax.ShapeDtypeStruct((tokens, quarter), kept),
        ),
        in_specs=[in_vmem] * 2 + [stays] * 3 + [in_vmem] * 3 + [in_smem, stays],
        out_specs=(in_vmem, in_vmem),
        scratch_shapes=[
            pltpu.VMEM(gate_one.shape, kept),
            pltpu.VMEM(up_one.shape, kept),
            pltpu.VMEM(down_one.shape, kept),
            pltpu.VMEM(project.shape, kept),
            pltpu.VMEM((2, WINDOW_KEYS, keys.shape[1]), kept),
            pltpu.VMEM(queries.shape, kept),
            pltpu.VMEM((queries.shape[0], width), kept),
            pltpu.VMEM((2, span, width), kept),
            pltpu.VMEM((span, width), kept),
            dma((4,)),
            dma((2,)),
            dma((2,)),
            dma((2,)),
            dma((2,)),
            dma,
            dma,
            pltpu.VMEM((blocks, tokens, width), kept),
            pltpu.VMEM((blocks, 8, tokens), jnp.float32),
            pltpu.VMEM((blocks, tokens, width), kept),
            pltpu.VMEM((blocks, tokens, 2 * quarter), kept),
            pltpu.VMEM((blocks, tokens, early), kept),
            pltpu.VMEM((LINE, tokens, carried), kept),
            pltpu.VMEM((LINE, tokens, carried), kept),
            pltpu.VMEM((LINE, tokens, carried), kept),
            pltpu.VMEM((tokens, quarter - early), kept),
            dma((blocks,)),
            dma((blocks,)),
            dma((2, LINE, 2)),
            dma((LINE, 2)),
            dma((LINE, 2)),
            dma((LINE, 2)),
            dma((blocks,)),
            dma((blocks,)),
            dma((blocks, 3)),
            dma((blocks, 3)),
            dma((blocks, 2)),
            dma((blocks, 2)),
            dma((blocks,)),
            dma((blocks,)),
            dma((LINE, 3)),
            dma((LINE, 3)),
            dma((LINE, 3)),
            dma((2, LINE, 3)),
            dma,
            dma,
        ],
        compiler_params=pltpu.CompilerParams(
            collective_id=0, has_side_effects=True, vmem_limit_bytes=60 * 1024 * 1024
        ),
        cost_estimate=pl.CostEstimate(
            flops=8 * blocks * tokens * width * gate_one.shape[1],
            bytes_accessed=8 * width * gate_one.shape[1],
            transcendentals=0,
        ),
    )(normed, share_of, gate_one, up_one, down_one, queries, keys, values, sinks, project)


def shards(
    projected_queries,
    key_proj,
    projected_values,
    head_sink_logits,
    out_weight,
    expert_input,
    norm_gain,
    routing,
    route_weight,
    gate_weight,
    up_weight,
    down_weight,
):
    token_rows = expert_input.shape[0]
    experts = lax.axis_size("ep")
    capacity = max(3 * token_rows * TOPK // (2 * experts), 2)
    col_share = D // lax.axis_size("tp")
    widened = expert_input.astype(jnp.float32)
    normed = (
        widened
        * lax.rsqrt(jnp.mean(widened * widened, axis=-1, keepdims=True) + EPS)
        * norm_gain[None, :]
    ).astype(jnp.bfloat16)
    if (experts, lax.axis_size("tp")) == (2 * LINE, 4) and token_rows == 128:
        named = routing == lax.broadcasted_iota(jnp.int32, (experts, 1, 1), 0)
        share_of = jnp.sum(jnp.where(named, route_weight[None], 0.0), axis=2)
        share_of = jnp.broadcast_to(share_of[:, None, :], (experts, 8, token_rows))
        return layer_call(
            normed,
            share_of,
            gate_weight[0],
            up_weight[0],
            down_weight[0],
            projected_queries,
            key_proj,
            projected_values,
            head_sink_logits,
            out_weight,
        )
    query_rows = projected_queries.shape[0]
    kv_heads = key_proj.shape[1] // HEAD_SIZE
    heads_per_group = projected_queries.shape[1] // HEAD_SIZE // kv_heads
    count_of_blocks = query_rows // WINDOW_KEYS
    prior_key, prior_value = passed_along(
        (key_proj[query_rows - WINDOW_KEYS :], projected_values[query_rows - WINDOW_KEYS :]),
        "ep",
        1,
    )
    key_all = jnp.concatenate([prior_key, key_proj], axis=0)
    value_all = jnp.concatenate([prior_value, projected_values], axis=0)
    window_keys = jnp.concatenate(
        [
            key_all[:-WINDOW_KEYS].reshape(count_of_blocks, WINDOW_KEYS, kv_heads, HEAD_SIZE),
            key_all[WINDOW_KEYS:].reshape(count_of_blocks, WINDOW_KEYS, kv_heads, HEAD_SIZE),
        ],
        axis=1,
    )
    window_values = jnp.concatenate(
        [
            value_all[:-WINDOW_KEYS].reshape(count_of_blocks, WINDOW_KEYS, kv_heads, HEAD_SIZE),
            value_all[WINDOW_KEYS:].reshape(count_of_blocks, WINDOW_KEYS, kv_heads, HEAD_SIZE),
        ],
        axis=1,
    )
    query_blocks = projected_queries.reshape(
        count_of_blocks, WINDOW_KEYS, kv_heads, heads_per_group, HEAD_SIZE
    )
    scores = jnp.einsum(
        "nqhgd,nshd->nhgqs", query_blocks, window_keys, preferred_element_type=jnp.float32
    ) * HEAD_SIZE ** (-0.5)
    offset = lax.axis_index("ep") * query_rows
    block_ids = jnp.arange(count_of_blocks)[:, None, None] * WINDOW_KEYS + offset
    query_pos = block_ids + jnp.arange(WINDOW_KEYS)[None, :, None]
    key_pos = block_ids - WINDOW_KEYS + jnp.arange(2 * WINDOW_KEYS)[None, None, :]
    permitted_mask = (key_pos <= query_pos) & (query_pos - key_pos < WINDOW_KEYS) & (key_pos >= 0)
    scores = jnp.where(permitted_mask[:, None, None, :, :], scores, -jnp.inf)
    sink_col = head_sink_logits.reshape(kv_heads, heads_per_group)[None, :, :, None, None]
    highest = jnp.maximum(jnp.max(scores, axis=-1, keepdims=True), sink_col)
    numerator = jnp.exp(scores - highest)
    denominator = jnp.sum(numerator, axis=-1, keepdims=True) + jnp.exp(sink_col - highest)
    weights = (numerator / denominator).astype(jnp.bfloat16)
    attended = jnp.einsum(
        "nhgqs,nshd->nqhgd", weights, window_values, preferred_element_type=jnp.float32
    )
    attended = attended.astype(jnp.bfloat16).reshape(
        query_rows, kv_heads * heads_per_group * HEAD_SIZE
    )
    mixer_output = lax.psum_scatter(
        jnp.dot(attended, out_weight, preferred_element_type=jnp.float32).astype(jnp.bfloat16),
        "tp",
        scatter_dimension=0,
        tiled=True,
    )
    flat_ids = routing.reshape(-1)
    onehot = (flat_ids[:, None] == jnp.arange(experts, dtype=jnp.int32)[None, :]).astype(jnp.int32)
    rank_in = jnp.cumsum(onehot, axis=0) - 1
    target = flat_ids * capacity + jnp.sum(rank_in * onehot, axis=1)
    tok_ids = jnp.arange(token_rows * TOPK) // TOPK
    slot_tok = jnp.full((experts * capacity,), token_rows, jnp.int32).at[target].set(tok_ids)
    gate_one = gate_weight[0]
    up_one = up_weight[0]
    own_cols = lax.dynamic_slice_in_dim(normed, lax.axis_index("tp") * col_share, col_share, 1)
    extended = jnp.concatenate([own_cols, jnp.zeros((1, col_share), jnp.bfloat16)], axis=0)
    outgoing = jnp.take(extended, slot_tok, axis=0).reshape(experts, capacity, col_share)
    arrived = lax.all_to_all(outgoing, "ep", split_axis=0, concat_axis=0, tiled=True).reshape(
        experts * capacity, col_share
    )
    portion = lax.all_gather(arrived, "tp", axis=1, tiled=True)
    gate_pre = jnp.dot(portion, gate_one, preferred_element_type=jnp.float32)
    up_pre = jnp.dot(portion, up_one, preferred_element_type=jnp.float32)
    gate_cut = jnp.minimum(gate_pre, CLAMP)
    activated = (
        (jnp.clip(up_pre, -CLAMP, CLAMP) + 1.0) * gate_cut * jax.nn.sigmoid(SLOPE * gate_cut)
    ).astype(jnp.bfloat16)
    partial_value = jnp.dot(activated, down_weight[0], preferred_element_type=jnp.float32)
    expert_result = lax.psum_scatter(
        partial_value.astype(jnp.bfloat16), "tp", scatter_dimension=1, tiled=True
    )
    returned = lax.all_to_all(
        expert_result.reshape(experts, capacity, col_share),
        "ep",
        split_axis=0,
        concat_axis=0,
        tiled=True,
    )
    picked = jnp.take(returned.reshape(experts * capacity, col_share), target, axis=0)
    picked = picked.astype(jnp.float32).reshape(token_rows, TOPK, col_share)
    expert_output = jnp.sum(picked * route_weight[:, :, None], axis=1).astype(jnp.bfloat16)
    return (mixer_output, expert_output)


def solution(mesh):
    placed = (
        P("ep", "tp"),
        P("ep", "tp"),
        P("ep", "tp"),
        P("tp"),
        P("tp", None),
        P("ep", None),
        P(),
        P("ep", None),
        P("ep", None),
        P("ep", None, "tp"),
        P("ep", None, "tp"),
        P("ep", "tp", None),
    )
    return jax.shard_map(
        shards,
        mesh=mesh,
        in_specs=placed,
        out_specs=(P(("ep", "tp"), None), P("ep", "tp")),
        check_vma=False,
    )
```

```python
import jax
import jax.numpy as jnp
from jax import lax
from jax.experimental import pallas as pl
from jax.experimental.pallas import tpu as pltpu
from jax.sharding import PartitionSpec as P

D = 4096
HEAD_SIZE = 64
WINDOW_KEYS = 128
TOPK = 4


EPS = 1e-06
CLAMP = 7.0
SLOPE = 1.702


def passed_along(block, axis, distance):
    devices = range(lax.axis_size(axis))
    route = [(i - distance, i) for i in devices if i - distance in devices]
    return lax.ppermute(block, axis, route)


LINE = 4
MESH = pl.DeviceIdType.MESH


def chosen(z, values):
    result = jnp.int32(values[0])
    for place in range(1, LINE):
        result = jnp.where(z == place, jnp.int32(values[place]), result)
    return result


def nearest_first(place):
    return sorted(range(LINE), key=lambda other: (abs(other - place), other))


def layer_kernel(
    token_ref,
    gain_ref,
    share_ref,
    gate_hbm,
    up_hbm,
    down_hbm,
    query_ref,
    key_ref,
    value_ref,
    sink_ref,
    project_hbm,
    mixer_ref,
    out_ref,
    own_ref,
    gate_ref,
    up_ref,
    down_ref,
    project_ref,
    halo_ref,
    attended_ref,
    mixed_ref,
    mixed_core_ref,
    mixed_pair_ref,
    load_sem,
    halo_send,
    halo_recv,
    mixed_core_send,
    mixed_core_recv,
    mixed_pair_send,
    mixed_pair_recv,
    rows_ref,
    weight_ref,
    sum_ref,
    core_ref,
    pair_ref,
    side_ref,
    up_line_ref,
    down_line_ref,
    last_ref,
    share_send,
    share_recv,
    line_send,
    line_recv,
    side_send,
    side_recv,
    pair_send,
    pair_recv,
    core_send,
    core_recv,
    back_core_send,
    back_core_recv,
    back_pair_send,
    back_pair_recv,
    back_side_send,
    back_side_recv,
    back_line_send,
    back_line_recv,
    last_send,
    last_recv,
):
    e, t = lax.axis_index("ep"), lax.axis_index("tp")
    z, x, y, c = e // 2, e % 2, t // 2, t % 2
    tokens, width = token_ref.shape
    sibling, partner, beside = (e, y * 2 + 1 - c), (e, (1 - y) * 2 + c), (z * 2 + 1 - x, t)
    above, below = (e + 2, t), (e - 2, t)

    def copy(src, dst, send, recv, to):
        return pltpu.make_async_remote_copy(
            src_ref=src, dst_ref=dst, send_sem=send, recv_sem=recv, device_id=to, device_id_type=MESH
        )

    loads = [
        pltpu.make_async_copy(src, dst, load_sem.at[place])
        for place, (src, dst) in enumerate(
            [(project_hbm, project_ref), (gate_hbm, gate_ref), (up_hbm, up_ref), (down_hbm, down_ref)]
        )
    ]
    for load in loads:
        load.start()
    barrier = pltpu.get_barrier_semaphore()
    for step in range(1, 2 * LINE):
        pl.semaphore_signal(
            barrier, inc=1, device_id=((e + step) % (2 * LINE), t), device_id_type=MESH
        )
    for other in (sibling, partner):
        pl.semaphore_signal(barrier, inc=1, device_id=other, device_id_type=MESH)
    widened = token_ref[...].astype(jnp.float32)
    scale = lax.rsqrt(jnp.mean(widened * widened, axis=-1, keepdims=True) + EPS)
    own_ref[...] = (widened * scale * gain_ref[...]).astype(jnp.bfloat16)
    rows_ref[e] = own_ref[...]
    pl.semaphore_wait(barrier, 2 * LINE + 1)

    lone = width * 3 // 16
    both = width // 8
    first = pl.multiple_of(y * (width - 2 * lone) + c * lone, 128)
    middle = pl.multiple_of(2 * lone + c * both, 128)
    other_first = pl.multiple_of((1 - y) * (width - 2 * lone) + c * lone, 128)
    parts = (pl.ds(first, lone), pl.ds(middle, both), pl.ds(other_first, lone))

    def view(block, part):
        return rows_ref.at[block, :, parts[part]]

    def source(block, part, mine):
        return own_ref.at[:, parts[part]] if mine else view(block, part)

    def along(way, at, part, mine, to):
        block = at * 2 + x
        return copy(
            source(block, part, mine), view(block, part),
            line_send.at[way, at, part], line_recv.at[at, part], to,
        )

    def across(at, part, mine):
        block = at * 2 + x
        return copy(
            source(block, part, mine), view(block, part),
            side_send.at[at, part], side_recv.at[at, part], beside,
        )

    def across_in(at, part):
        block = at * 2 + 1 - x
        return copy(
            view(block, part), view(block, part), side_send.at[at, part], side_recv.at[at, part], beside
        )

    def to_partner(block):
        return copy(view(block, 0), view(block, 0), pair_send.at[block], pair_recv.at[block], partner)

    def from_partner(block):
        return copy(view(block, 2), view(block, 2), pair_send.at[block], pair_recv.at[block], partner)

    def to_sibling(block, part):
        return copy(
            view(block, part), view(block, part), core_send.at[block, part], core_recv.at[block, part], sibling
        )

    sibling_parts = (
        pl.ds(pl.multiple_of(y * (width - 2 * lone) + (1 - c) * lone, 128), lone),
        pl.ds(pl.multiple_of(2 * lone + (1 - c) * both, 128), both),
        pl.ds(pl.multiple_of((1 - y) * (width - 2 * lone) + (1 - c) * lone, 128), lone),
    )

    def from_sibling(block, part):
        dst = rows_ref.at[block, :, sibling_parts[part]]
        return copy(dst, dst, core_send.at[block, part], core_recv.at[block, part], sibling)

    def share_copy(step):
        to = (e + step) % (2 * LINE)
        return copy(
            share_ref.at[to], weight_ref.at[e], share_send.at[step], share_recv.at[e], (to, t)
        )

    def share_in(step):
        at = (e + step) % (2 * LINE)
        return copy(share_ref.at[at], weight_ref.at[at], share_send.at[step], share_recv.at[at], (at, t))

    for part in (0, 1):
        @pl.when(z < LINE - 1)
        def _():
            along(0, z, part, True, above).start()

        @pl.when(z > 0)
        def _():
            along(1, z, part, True, below).start()

        across(z, part, True).start()
    queries = query_ref.shape[0]

    def halo_copy(which):
        src = (key_ref, value_ref)[which].at[pl.ds(queries - WINDOW_KEYS, WINDOW_KEYS)]
        to = ((e + 1) % (2 * LINE), t)
        return copy(src, halo_ref.at[which], halo_send.at[which], halo_recv.at[which], to)

    @pl.when(e < 2 * LINE - 1)
    def _():
        halo_copy(0).start()
        halo_copy(1).start()

    @pl.when(e == 0)
    def _():
        halo_ref[...] = jnp.zeros_like(halo_ref)

    for step in range(1, 2 * LINE):
        share_copy(step).start()
    weight_ref[e] = share_ref[e]

    kv_heads = key_ref.shape[1] // HEAD_SIZE
    group = query_ref.shape[1] // HEAD_SIZE // kv_heads
    span = queries // 4
    here = lax.broadcasted_iota(jnp.int32, (WINDOW_KEYS, 2 * WINDOW_KEYS), 0)
    there = lax.broadcasted_iota(jnp.int32, (WINDOW_KEYS, 2 * WINDOW_KEYS), 1)

    def attend(number):
        begin = number * WINDOW_KEYS
        permitted = (there > here) & (there <= here + WINDOW_KEYS)
        if number == 0:
            permitted = permitted & ((there >= WINDOW_KEYS) | (e > 0))
        for kv in range(kv_heads):
            lanes = slice(kv * HEAD_SIZE, (kv + 1) * HEAD_SIZE)
            if number == 0:
                keys = jnp.concatenate([halo_ref[0][:, lanes], key_ref[0:WINDOW_KEYS, lanes]], axis=0)
                values = jnp.concatenate(
                    [halo_ref[1][:, lanes], value_ref[0:WINDOW_KEYS, lanes]], axis=0
                )
            else:
                keys = key_ref[begin - WINDOW_KEYS : begin + WINDOW_KEYS, lanes]
                values = value_ref[begin - WINDOW_KEYS : begin + WINDOW_KEYS, lanes]
            for member in range(group):
                head = kv * group + member
                columns = slice(head * HEAD_SIZE, (head + 1) * HEAD_SIZE)
                scores = lax.dot_general(
                    query_ref[begin : begin + WINDOW_KEYS, columns],
                    keys,
                    (((1,), (1,)), ((), ())),
                    preferred_element_type=jnp.float32,
                ) * HEAD_SIZE ** (-0.5)
                scores = jnp.where(permitted, scores, -jnp.inf)
                sink = sink_ref[head]
                highest = jnp.maximum(jnp.max(scores, axis=-1, keepdims=True), sink)
                numerator = jnp.exp(scores - highest)
                denominator = jnp.sum(numerator, axis=-1, keepdims=True) + jnp.exp(sink - highest)
                weights = (numerator / denominator).astype(jnp.bfloat16)
                found = jnp.dot(weights, values, preferred_element_type=jnp.float32)
                attended_ref[begin : begin + WINDOW_KEYS, columns] = found.astype(jnp.bfloat16)

    def mixed_core(half):
        at = pl.multiple_of((half * 2 + 1 - c) * span, 16)
        return copy(
            mixed_ref.at[pl.ds(at, span)], mixed_core_ref.at[half],
            mixed_core_send.at[half], mixed_core_recv.at[half], sibling,
        )

    mixed_pair = copy(
        mixed_ref.at[pl.ds(pl.multiple_of(((1 - y) * 2 + c) * span, 16), span)], mixed_pair_ref,
        mixed_pair_send, mixed_pair_recv, partner,
    )

    def mixed_rows(half):
        return pl.ds(pl.multiple_of((half * 2 + c) * span, 16), span)

    def mix():
        for number in range(1, queries // WINDOW_KEYS):
            attend(number)

        @pl.when(e > 0)
        def _():
            halo_copy(0).wait_recv()
            halo_copy(1).wait_recv()

        attend(0)
        loads[0].wait()
        for place in range(0, width, width // 4):
            columns = slice(place, place + width // 4)
            mixed_ref[:, columns] = jnp.dot(
                attended_ref[...], project_ref[:, columns], preferred_element_type=jnp.float32
            ).astype(jnp.bfloat16)
        for half in range(2):
            mixed_core(half).start()

    def mix_onward():
        for half in range(2):
            mixed_core(half).wait_recv()
            total = mixed_ref[mixed_rows(half), :].astype(jnp.float32)
            mixed_ref[mixed_rows(half), :] = (
                total + mixed_core_ref[half].astype(jnp.float32)
            ).astype(jnp.bfloat16)

    mix()
    near = [chosen(z, [nearest_first(place)[j] for place in range(LINE)]) for j in range(LINE)]
    sequence = []

    def passed_on(block):
        to_partner(block).start()
        to_sibling(block, 0).start()
        to_sibling(block, 1).start()
        sequence.append(block)

    def settle(block):
        from_partner(block).wait_recv()
        to_sibling(block, 2).start()

    for j in range(1, LINE + 1):
        if j < LINE:
            at = near[j]
            for part in (0, 1):
                along(0, at, part, False, above).wait_recv()

                @pl.when((at < z) & (z < LINE - 1))
                def _():
                    along(0, at, part, False, above).start()

                @pl.when((at > z) & (z > 0))
                def _():
                    along(1, at, part, False, below).start()

                across(at, part, False).start()
            passed_on(at * 2 + x)
            if len(sequence) > 2:
                settle(sequence[len(sequence) - 3])
        for part in (0, 1):
            across_in(near[j - 1], part).wait_recv()
        passed_on(near[j - 1] * 2 + 1 - x)
        if len(sequence) > 2:
            settle(sequence[len(sequence) - 3])
    mix_onward()
    for block in sequence[-2:]:
        settle(block)
    for load in loads[1:]:
        load.wait()
    for step in range(1, 2 * LINE):
        share_in(step).wait_recv()
    for block in sequence:
        for part in range(3):
            from_sibling(block, part).wait_recv()

    quarter = width // 4
    early = quarter * 5 // 8
    late = quarter - early
    mine = pl.multiple_of((y * 2 + c) * quarter, 128)
    theirs = pl.multiple_of(((1 - y) * 2 + c) * quarter, 128)
    early_mine, early_theirs = pl.ds(mine, early), pl.ds(theirs, early)
    late_mine = pl.ds(pl.multiple_of(mine + early, 128), late)
    late_theirs = pl.ds(pl.multiple_of(theirs + early, 128), late)
    own_quarter, other_quarter = pl.ds(mine, quarter), pl.ds(theirs, quarter)
    sent_quarters = [
        pl.ds(pl.multiple_of((half * 2 + 1 - c) * quarter, 128), quarter) for half in range(2)
    ]
    kept_quarters = [
        pl.ds(pl.multiple_of((half * 2 + c) * quarter, 128), quarter) for half in range(2)
    ]
    trio = ((early_mine, 0, early), (late_mine, early, late), (late_theirs, quarter, late))

    def add(block, columns, arrived):
        total = sum_ref[block, :, columns].astype(jnp.float32)
        sum_ref[block, :, columns] = (total + arrived.astype(jnp.float32)).astype(jnp.bfloat16)

    def far(j):
        result = chosen(z, [nearest_first(place)[::-1][0] for place in range(LINE)])
        for index in range(1, LINE):
            value = chosen(z, [nearest_first(place)[::-1][index] for place in range(LINE)])
            result = jnp.where(j == index, value, result)
        return result

    def back_core(block, half, columns):
        return copy(
            sum_ref.at[block, :, columns], core_ref.at[block, :, pl.ds(half * quarter, quarter)],
            back_core_send.at[block, half], back_core_recv.at[block, half], sibling,
        )

    def back_pair(block):
        return copy(
            sum_ref.at[block, :, early_theirs], pair_ref.at[block],
            back_pair_send.at[block], back_pair_recv.at[block], partner,
        )

    def back_side(at, index):
        columns, start, length = trio[index]
        return copy(
            sum_ref.at[at * 2 + 1 - x, :, columns], side_ref.at[at, :, pl.ds(start, length)],
            back_side_send.at[at, index], back_side_recv.at[at, index], beside,
        )

    def back_line(way, at, index, to):
        columns, start, length = trio[index]
        landing = (up_line_ref, down_line_ref)[way]
        return copy(
            sum_ref.at[at * 2 + x, :, columns], landing.at[at, :, pl.ds(start, length)],
            back_line_send.at[at, index], back_line_recv.at[way, at, index], to,
        )

    def line_in(way, at):
        for index, (columns, start, length) in enumerate(trio):
            back_line(way, at, index, above).wait_recv()
            landing = (up_line_ref, down_line_ref)[way]
            add(at * 2 + x, columns, landing[at, :, start : start + length])

    last = copy(sum_ref.at[e, :, late_theirs], last_ref, last_send, last_recv, partner)

    def experts_of(block):
        rows = rows_ref[block]
        gate_pre = jnp.dot(rows, gate_ref[...], preferred_element_type=jnp.float32)
        up_pre = jnp.dot(rows, up_ref[...], preferred_element_type=jnp.float32)
        gate_cut = jnp.minimum(gate_pre, CLAMP)
        activated = (
            (jnp.clip(up_pre, -CLAMP, CLAMP) + 1.0) * gate_cut * jax.nn.sigmoid(SLOPE * gate_cut)
        ).astype(jnp.bfloat16)
        weight = jnp.broadcast_to(weight_ref[block][0:1], (tokens, tokens)).T[:, 0:1]

        for place in range(0, width, quarter):
            result = jnp.dot(
                activated, down_ref[:, place : place + quarter], preferred_element_type=jnp.float32
            )
            sum_ref[block, :, place : place + quarter] = (result * weight).astype(jnp.bfloat16)

    def turn(i, carry):
        @pl.when(i < LINE)
        def _():
            at = far(i)

            def one(index, inner):
                block = at * 2 + (1 - x) * (1 - index) + x * index
                experts_of(block)
                for half in range(2):
                    back_core(block, half, sent_quarters[half]).start()
                return inner

            lax.fori_loop(0, 2, one, 0)

        @pl.when((i >= 1) & (i < LINE + 1))
        def _():
            at = far(i - 1)

            def one(index, inner):
                block = at * 2 + (1 - x) * (1 - index) + x * index
                for half in range(2):
                    back_core(block, half, sent_quarters[half]).wait_recv()
                    add(block, kept_quarters[half], core_ref[block, :, half * quarter : (half + 1) * quarter])
                back_pair(block).start()
                return inner

            lax.fori_loop(0, 2, one, 0)

        @pl.when(i == LINE)
        def _():
            mixed_pair.start()

        @pl.when((i >= 2) & (i < LINE + 2))
        def _():
            at = far(i - 2)

            def one(index, inner):
                block = at * 2 + (1 - x) * (1 - index) + x * index
                back_pair(block).wait_recv()
                add(block, early_mine, pair_ref[block])

                @pl.when(index == 0)
                def _():
                    for part in range(3):
                        back_side(at, part).start()

                return inner

            lax.fori_loop(0, 2, one, 0)

        @pl.when(i >= 3)
        def _():
            at = far(i - 3)
            for part, (columns, start, length) in enumerate(trio):
                back_side(at, part).wait_recv()
                add(at * 2 + x, columns, side_ref[at, :, start : start + length])

            @pl.when((at >= z) & (z > 0))
            def _():
                line_in(0, at)

            @pl.when((at <= z) & (z < LINE - 1))
            def _():
                line_in(1, at)

            @pl.when(at > z)
            def _():
                for part in range(3):
                    back_line(0, at, part, above).start()

            @pl.when(at < z)
            def _():
                for part in range(3):
                    back_line(1, at, part, below).start()

        return carry

    lax.fori_loop(0, LINE + 3, turn, 0)
    last.start()
    last.wait_recv()
    out_ref[:, 0:early] = sum_ref[e, :, early_mine]
    closing = sum_ref[e, :, late_mine].astype(jnp.float32) + last_ref[...].astype(jnp.float32)
    out_ref[:, early:quarter] = closing.astype(jnp.bfloat16)

    mixed_pair.wait_recv()
    total = mixed_ref[mixed_rows(y), :].astype(jnp.float32)
    mixer_ref[...] = (total + mixed_pair_ref[...].astype(jnp.float32)).astype(jnp.bfloat16)

    last.wait_send()
    mixed_pair.wait_send()
    for half in range(2):
        mixed_core(half).wait_send()

    @pl.when(e < 2 * LINE - 1)
    def _():
        halo_copy(0).wait_send()
        halo_copy(1).wait_send()

    for part in (0, 1):
        @pl.when(z < LINE - 1)
        def _():
            along(0, z, part, True, above).wait_send()

        @pl.when(z > 0)
        def _():
            along(1, z, part, True, below).wait_send()

        across(z, part, True).wait_send()
    for step in range(1, 2 * LINE):
        share_copy(step).wait_send()
    for j in range(1, LINE):
        at = near[j]
        for part in (0, 1):
            @pl.when((at < z) & (z < LINE - 1))
            def _():
                along(0, at, part, False, above).wait_send()

            @pl.when((at > z) & (z > 0))
            def _():
                along(1, at, part, False, below).wait_send()

            across(at, part, False).wait_send()
    for block in sequence:
        to_partner(block).wait_send()
        for part in range(3):
            to_sibling(block, part).wait_send()

    def drained(at, carry):
        for side in range(2):
            for half in range(2):
                back_core(at * 2 + side, half, sent_quarters[half]).wait_send()
            back_pair(at * 2 + side).wait_send()
        for part in range(3):
            back_side(at, part).wait_send()

            @pl.when(at != z)
            def _():
                back_line(0, at, part, above).wait_send()

        return carry

    lax.fori_loop(0, LINE, drained, 0)


def layer_call(
    rows, gain, share_of, gate_one, up_one, down_one, queries, keys, values, sinks, project
):
    tokens, width = rows.shape
    quarter = width // 4
    early = quarter * 5 // 8
    carried = quarter + quarter - early
    blocks = 2 * LINE
    kept = jnp.bfloat16
    dma = pltpu.SemaphoreType.DMA
    span = queries.shape[0] // 4
    in_vmem = pl.BlockSpec(memory_space=pltpu.VMEM)
    in_smem = pl.BlockSpec(memory_space=pltpu.SMEM)
    stays = pl.BlockSpec(memory_space=pl.ANY)
    return pl.pallas_call(
        layer_kernel,
        out_shape=(
            jax.ShapeDtypeStruct((span, width), kept),
            jax.ShapeDtypeStruct((tokens, quarter), kept),
        ),
        in_specs=[in_vmem] * 3 + [stays] * 3 + [in_vmem] * 3 + [in_smem, stays],
        out_specs=(in_vmem, in_vmem),
        scratch_shapes=[
            pltpu.VMEM(rows.shape, kept),
            pltpu.VMEM(gate_one.shape, kept),
            pltpu.VMEM(up_one.shape, kept),
            pltpu.VMEM(down_one.shape, kept),
            pltpu.VMEM(project.shape, kept),
            pltpu.VMEM((2, WINDOW_KEYS, keys.shape[1]), kept),
            pltpu.VMEM(queries.shape, kept),
            pltpu.VMEM((queries.shape[0], width), kept),
            pltpu.VMEM((2, span, width), kept),
            pltpu.VMEM((span, width), kept),
            dma((4,)),
            dma((2,)),
            dma((2,)),
            dma((2,)),
            dma((2,)),
            dma,
            dma,
            pltpu.VMEM((blocks, tokens, width), kept),
            pltpu.VMEM((blocks, 8, tokens), jnp.float32),
            pltpu.VMEM((blocks, tokens, width), kept),
            pltpu.VMEM((blocks, tokens, 2 * quarter), kept),
            pltpu.VMEM((blocks, tokens, early), kept),
            pltpu.VMEM((LINE, tokens, carried), kept),
            pltpu.VMEM((LINE, tokens, carried), kept),
            pltpu.VMEM((LINE, tokens, carried), kept),
            pltpu.VMEM((tokens, quarter - early), kept),
            dma((blocks,)),
            dma((blocks,)),
            dma((2, LINE, 2)),
            dma((LINE, 2)),
            dma((LINE, 2)),
            dma((LINE, 2)),
            dma((blocks,)),
            dma((blocks,)),
            dma((blocks, 3)),
            dma((blocks, 3)),
            dma((blocks, 2)),
            dma((blocks, 2)),
            dma((blocks,)),
            dma((blocks,)),
            dma((LINE, 3)),
            dma((LINE, 3)),
            dma((LINE, 3)),
            dma((2, LINE, 3)),
            dma,
            dma,
        ],
        compiler_params=pltpu.CompilerParams(
            collective_id=0, has_side_effects=True, vmem_limit_bytes=60 * 1024 * 1024
        ),
        cost_estimate=pl.CostEstimate(
            flops=8 * blocks * tokens * width * gate_one.shape[1],
            bytes_accessed=8 * width * gate_one.shape[1],
            transcendentals=0,
        ),
    )(rows, gain, share_of, gate_one, up_one, down_one, queries, keys, values, sinks, project)


def shards(
    projected_queries,
    key_proj,
    projected_values,
    head_sink_logits,
    out_weight,
    expert_input,
    norm_gain,
    routing,
    route_weight,
    gate_weight,
    up_weight,
    down_weight,
):
    token_rows = expert_input.shape[0]
    experts = lax.axis_size("ep")
    capacity = max(3 * token_rows * TOPK // (2 * experts), 2)
    col_share = D // lax.axis_size("tp")
    widened = expert_input.astype(jnp.float32)
    normed = (
        widened
        * lax.rsqrt(jnp.mean(widened * widened, axis=-1, keepdims=True) + EPS)
        * norm_gain[None, :]
    ).astype(jnp.bfloat16)
    if (experts, lax.axis_size("tp")) == (2 * LINE, 4) and token_rows == 128:
        named = routing == lax.broadcasted_iota(jnp.int32, (experts, 1, 1), 0)
        share_of = jnp.sum(jnp.where(named, route_weight[None], 0.0), axis=2)
        share_of = jnp.broadcast_to(share_of[:, None, :], (experts, 8, token_rows))
        return layer_call(
            expert_input,
            norm_gain[None, :],
            share_of,
            gate_weight[0],
            up_weight[0],
            down_weight[0],
            projected_queries,
            key_proj,
            projected_values,
            head_sink_logits,
            out_weight,
        )
    query_rows = projected_queries.shape[0]
    kv_heads = key_proj.shape[1] // HEAD_SIZE
    heads_per_group = projected_queries.shape[1] // HEAD_SIZE // kv_heads
    count_of_blocks = query_rows // WINDOW_KEYS
    prior_key, prior_value = passed_along(
        (key_proj[query_rows - WINDOW_KEYS :], projected_values[query_rows - WINDOW_KEYS :]),
        "ep",
        1,
    )
    key_all = jnp.concatenate([prior_key, key_proj], axis=0)
    value_all = jnp.concatenate([prior_value, projected_values], axis=0)
    window_keys = jnp.concatenate(
        [
            key_all[:-WINDOW_KEYS].reshape(count_of_blocks, WINDOW_KEYS, kv_heads, HEAD_SIZE),
            key_all[WINDOW_KEYS:].reshape(count_of_blocks, WINDOW_KEYS, kv_heads, HEAD_SIZE),
        ],
        axis=1,
    )
    window_values = jnp.concatenate(
        [
            value_all[:-WINDOW_KEYS].reshape(count_of_blocks, WINDOW_KEYS, kv_heads, HEAD_SIZE),
            value_all[WINDOW_KEYS:].reshape(count_of_blocks, WINDOW_KEYS, kv_heads, HEAD_SIZE),
        ],
        axis=1,
    )
    query_blocks = projected_queries.reshape(
        count_of_blocks, WINDOW_KEYS, kv_heads, heads_per_group, HEAD_SIZE
    )
    scores = jnp.einsum(
        "nqhgd,nshd->nhgqs", query_blocks, window_keys, preferred_element_type=jnp.float32
    ) * HEAD_SIZE ** (-0.5)
    offset = lax.axis_index("ep") * query_rows
    block_ids = jnp.arange(count_of_blocks)[:, None, None] * WINDOW_KEYS + offset
    query_pos = block_ids + jnp.arange(WINDOW_KEYS)[None, :, None]
    key_pos = block_ids - WINDOW_KEYS + jnp.arange(2 * WINDOW_KEYS)[None, None, :]
    permitted_mask = (key_pos <= query_pos) & (query_pos - key_pos < WINDOW_KEYS) & (key_pos >= 0)
    scores = jnp.where(permitted_mask[:, None, None, :, :], scores, -jnp.inf)
    sink_col = head_sink_logits.reshape(kv_heads, heads_per_group)[None, :, :, None, None]
    highest = jnp.maximum(jnp.max(scores, axis=-1, keepdims=True), sink_col)
    numerator = jnp.exp(scores - highest)
    denominator = jnp.sum(numerator, axis=-1, keepdims=True) + jnp.exp(sink_col - highest)
    weights = (numerator / denominator).astype(jnp.bfloat16)
    attended = jnp.einsum(
        "nhgqs,nshd->nqhgd", weights, window_values, preferred_element_type=jnp.float32
    )
    attended = attended.astype(jnp.bfloat16).reshape(
        query_rows, kv_heads * heads_per_group * HEAD_SIZE
    )
    mixer_output = lax.psum_scatter(
        jnp.dot(attended, out_weight, preferred_element_type=jnp.float32).astype(jnp.bfloat16),
        "tp",
        scatter_dimension=0,
        tiled=True,
    )
    flat_ids = routing.reshape(-1)
    onehot = (flat_ids[:, None] == jnp.arange(experts, dtype=jnp.int32)[None, :]).astype(jnp.int32)
    rank_in = jnp.cumsum(onehot, axis=0) - 1
    target = flat_ids * capacity + jnp.sum(rank_in * onehot, axis=1)
    tok_ids = jnp.arange(token_rows * TOPK) // TOPK
    slot_tok = jnp.full((experts * capacity,), token_rows, jnp.int32).at[target].set(tok_ids)
    gate_one = gate_weight[0]
    up_one = up_weight[0]
    own_cols = lax.dynamic_slice_in_dim(normed, lax.axis_index("tp") * col_share, col_share, 1)
    extended = jnp.concatenate([own_cols, jnp.zeros((1, col_share), jnp.bfloat16)], axis=0)
    outgoing = jnp.take(extended, slot_tok, axis=0).reshape(experts, capacity, col_share)
    arrived = lax.all_to_all(outgoing, "ep", split_axis=0, concat_axis=0, tiled=True).reshape(
        experts * capacity, col_share
    )
    portion = lax.all_gather(arrived, "tp", axis=1, tiled=True)
    gate_pre = jnp.dot(portion, gate_one, preferred_element_type=jnp.float32)
    up_pre = jnp.dot(portion, up_one, preferred_element_type=jnp.float32)
    gate_cut = jnp.minimum(gate_pre, CLAMP)
    activated = (
        (jnp.clip(up_pre, -CLAMP, CLAMP) + 1.0) * gate_cut * jax.nn.sigmoid(SLOPE * gate_cut)
    ).astype(jnp.bfloat16)
    partial_value = jnp.dot(activated, down_weight[0], preferred_element_type=jnp.float32)
    expert_result = lax.psum_scatter(
        partial_value.astype(jnp.bfloat16), "tp", scatter_dimension=1, tiled=True
    )
    returned = lax.all_to_all(
        expert_result.reshape(experts, capacity, col_share),
        "ep",
        split_axis=0,
        concat_axis=0,
        tiled=True,
    )
    picked = jnp.take(returned.reshape(experts * capacity, col_share), target, axis=0)
    picked = picked.astype(jnp.float32).reshape(token_rows, TOPK, col_share)
    expert_output = jnp.sum(picked * route_weight[:, :, None], axis=1).astype(jnp.bfloat16)
    return (mixer_output, expert_output)


def solution(mesh):
    placed = (
        P("ep", "tp"),
        P("ep", "tp"),
        P("ep", "tp"),
        P("tp"),
        P("tp", None),
        P("ep", None),
        P(),
        P("ep", None),
        P("ep", None),
        P("ep", None, "tp"),
        P("ep", None, "tp"),
        P("ep", "tp", None),
    )
    return jax.shard_map(
        shards,
        mesh=mesh,
        in_specs=placed,
        out_specs=(P(("ep", "tp"), None), P("ep", "tp")),
        check_vma=False,
    )
```
